768 devices in a mesh: sp: 16 (over y, core), dp: 48 (over z, x).
Axes of the slice: x: 4, y: 8, z: 12, core: 2. Of those that a mesh axis runs over, the one named last changes fastest.
Arguments:
- queries: bfloat16 [48, 2048, 2048], P('dp', 'sp'), may hold values from -6 to 6
- incoming_lookup_vectors: bfloat16 [48, 2048, 2048], P('dp', 'sp'), may hold values from -6 to 6
- values_in: bfloat16 [48, 2048, 2048], P('dp', 'sp'), may hold values from -6 to 6
- gates: bfloat16 [48, 2048, 2048], P('dp', 'sp'), may hold values from -6 to 6
- log_decay: float32 [48, 16, 2048], P('dp', 'sp'), may hold values from -1 to 0
- out_weight: bfloat16 [2048, 2048], P(None, 'sp'), may hold values from -0.125 to 0.125
Outputs:
- mixed: bfloat16 [48, 2048, 2048], P('dp', 'sp')
The draws below stay inside these ranges and needn't reach their ends.
All inputs are finite; a program needn't handle non-finite values.
Results may differ from the reference program's by a relative error of at most 0.0057.
Values may be sent and summed in bfloat16 or wider, within the bound.
A program may use at most 64 MiB of HBM per device.

```python
import math
import jax
import jax.numpy as jnp
from jax import lax

TOK_DEV = 128
HEADS = 16
D = 2048
BLOCK = 128
WIDTH = 2048
TOTAL_STEP_COUNT = 2048
BATCH = 48


def draw_log_decay(key, part):
    keys = jax.random.split(key, 6)
    fast_fraction = 0.5
    fast = jax.random.uniform(keys[0], (BATCH, HEADS, 1), jnp.float32) < fast_fraction
    fast_rate = -1.0 / jax.random.uniform(keys[1], (BATCH, HEADS, 1), jnp.float32, 30.0, 50.0)
    slow_rate = -jax.random.uniform(keys[2], (BATCH, HEADS, 1), jnp.float32, 0.15, 0.5) / TOTAL_STEP_COUNT
    pieces = TOTAL_STEP_COUNT // TOK_DEV
    pace = jnp.exp(jax.random.uniform(keys[3], (BATCH, 1, pieces), jnp.float32, 0.0, math.log(4.0)))
    pace = jnp.repeat(pace, TOK_DEV, axis=2)
    forgetting_factor = jnp.where(fast, fast_rate, slow_rate) * pace
    slot_number = jax.random.randint(keys[4], (BATCH, 3), 0, TOTAL_STEP_COUNT)
    sudden_spots = jnp.any(jnp.arange(TOTAL_STEP_COUNT)[None, None, :] == slot_number[:, :, None], axis=1)[:, None, :]
    stack_level = jnp.log(jax.random.uniform(keys[5], (BATCH, HEADS, TOTAL_STEP_COUNT), jnp.float32, 0.5, 0.8))
    return forgetting_factor + jnp.where(sudden_spots, stack_level, 0.0)


def block_scale(own_key, shape, cuts, low, top_value):
    factor_of, own = 1.0, jax.random.fold_in(own_key, 6)
    for dim, blocks in cuts:
        draws = jnp.exp(jax.random.uniform(jax.random.fold_in(own, dim), (blocks,), jnp.float32, low / len(cuts), top_value / len(cuts)))
        factor_of = factor_of * jnp.repeat(draws, shape[dim] // blocks).reshape([-1 if axis == dim else 1 for axis in range(len(shape))])
    return factor_of


def gaussian(key, shape, scale, most, cuts=(), kind=jnp.bfloat16):
    gain = block_scale(key, shape, cuts, -0.22, 0.18) if cuts else 1.0
    values = jax.random.normal(key, shape, jnp.float32) * scale * gain
    return jnp.minimum(jnp.maximum(values, -most), most).astype(kind)


def setup_inputs(seed: int = 0) -> dict:
    splits = jax.random.split(jax.random.key(seed), 7)
    queries = gaussian(splits[0], (BATCH, TOTAL_STEP_COUNT, WIDTH), 1.0, 6.0, ((0, 48), (1, 16)))
    incoming_lookup_vectors = gaussian(splits[1], (BATCH, TOTAL_STEP_COUNT, WIDTH), 1.0, 6.0, ((0, 48), (1, 16)))
    values_in = gaussian(splits[2], (BATCH, TOTAL_STEP_COUNT, WIDTH), 1.0, 6.0, ((0, 48), (1, 16)))
    gates = gaussian(splits[3], (BATCH, TOTAL_STEP_COUNT, WIDTH), 1.0, 6.0, ((0, 48), (1, 16)))
    log_decay = draw_log_decay(jax.random.fold_in(splits[6], 71), 0)
    out_weight = gaussian(splits[5], (WIDTH, D), WIDTH ** -0.5, 0.125, ((1, 16),))
    return dict(queries=queries, incoming_lookup_vectors=incoming_lookup_vectors, values_in=values_in, gates=gates, log_decay=log_decay, out_weight=out_weight)


EPS = 1e-06
ROTARY_BASE = 10000.0

def rotary(field, head_size):
    half = head_size // 2
    inverse = ROTARY_BASE ** (-jnp.arange(half, dtype=jnp.float32) / half)
    angle = jnp.arange(field.shape[0], dtype=jnp.float32)[:, None] * inverse
    cosine = jnp.cos(angle)[:, None, :]
    sine = jnp.sin(angle)[:, None, :]
    first = field[..., :half]
    latter_operand = field[..., half:]
    return jnp.concatenate([first * cosine - latter_operand * sine, first * sine + latter_operand * cosine], axis=-1)

def retain(query, keyed, value_rows, decay, span):
    length, heads, size = query.shape
    blocks = length // span
    high = lax.Precision.HIGHEST
    qb = query.reshape(blocks, span, heads, size).transpose(2, 0, 1, 3)
    kb = keyed.reshape(blocks, span, heads, size).transpose(2, 0, 1, 3)
    vb = value_rows.reshape(blocks, span, heads, size).transpose(2, 0, 1, 3)
    summed = jnp.cumsum(decay.reshape(heads, blocks, span), axis=-1)
    spread = summed[..., :, None] - summed[..., None, :]
    place = jnp.arange(span)
    causal = place[:, None] >= place[None, :]
    weight = jnp.exp(jnp.where(causal, spread, -jnp.inf))
    scores = jnp.einsum('hnid,hnjd->hnij', qb, kb, precision=high) * weight
    inner = jnp.einsum('hnij,hnje->hnie', scores, vb, precision=high)
    final = summed[..., -1:]
    faded = kb * jnp.exp(final - summed)[..., None]
    growth = jnp.einsum('hnjd,hnje->nhde', faded, vb, precision=high)
    carried = jnp.exp(final[..., 0]).T

    def advance(state, item):
        piece, fade = item
        return (state * fade[:, None, None] + piece, state)
    start = jnp.zeros((heads, size, size), jnp.float32)
    _, earlier_positions = lax.scan(advance, start, (growth, carried))
    lifted = qb * jnp.exp(summed)[..., None]
    cross = jnp.einsum('hnid,nhde->hnie', lifted, earlier_positions, precision=high)
    return (inner + cross).transpose(1, 2, 0, 3).reshape(length, heads, size)

def reference(queries, incoming_lookup_vectors, values_in, gates, log_decay, out_weight):

    def one_sequence(args):
        query, keyed, value_rows, gate, decay = args
        heads = decay.shape[0]
        length = query.shape[0]
        size = query.shape[1] // heads
        qf = rotary(query.astype(jnp.float32).reshape(length, heads, size), size)
        kf = rotary(keyed.astype(jnp.float32).reshape(length, heads, size), size)
        vf = value_rows.astype(jnp.float32).reshape(length, heads, size)
        result = retain(qf, kf, vf, decay, BLOCK)
        result = result * lax.rsqrt(lax.optimization_barrier(jnp.mean(result * result, axis=-1, keepdims=True)) + EPS)
        normed = result.reshape(length, heads * size).astype(jnp.bfloat16)
        hidden = (normed.astype(jnp.float32) * jax.nn.silu(gate.astype(jnp.float32))).astype(jnp.bfloat16)
        return jnp.dot(hidden, out_weight, preferred_element_type=jnp.float32).astype(jnp.bfloat16)
    return lax.map(one_sequence, (queries, incoming_lookup_vectors, values_in, gates, log_decay))
```

```python
import functools
import math

import jax
import jax.numpy as jnp
from jax import lax
from jax.experimental import pallas as pl
from jax.experimental.pallas import tpu as pltpu
from jax.sharding import PartitionSpec as P

EPS = 1e-06
ROTARY_BASE = 10000.0
MESH = pl.DeviceIdType.MESH
F32, BF16 = jnp.float32, jnp.bfloat16
NX, NZ, NY = 4, 12, 8
HEADS, SIZE, TOK, HALF = 16, 128, 128, 8
SPAN = 2 * TOK
LANE = HALF * SIZE
PIECE = LANE // 4


def split(x):
    high = x.astype(BF16)
    return high, (x - high.astype(F32)).astype(BF16)


def dot(a, b, ca, cb):
    return lax.dot_general(a, b, (((ca,), (cb,)), ((), ())), preferred_element_type=F32)


def exact(a, b, ca, cb):
    return lax.dot_general(
        a,
        b,
        (((ca,), (cb,)), ((), ())),
        precision=lax.Precision.HIGHEST,
        preferred_element_type=F32,
    )


def kernel(
    q_ref, k_ref, v_ref, g_ref, ld_ref, w_ref, out_ref,
    x_buf, row_buf, dec, w_buf, cos_t, sin_t, col_buf, sum_buf, qrot, krot, inner,
    g_send, g_recv, s_send, s_recv, state, hidden, p_send, p_own, p_recv,
    load_sem, w_load_sem, row_sem, xs_sem, xr_sem, ds_sem, dr_sem, ws_sem, wr_sem,
    ys_sem, yr_sem, ns_sem, nr_sem, gs_sem, gr_sem, ss_sem, sr_sem, ps_sem, pr_sem,
):
    sp = lax.axis_index("sp")
    dp = lax.axis_index("dp")
    y, c = lax.div(sp, 2), lax.rem(sp, 2)
    z, x = lax.div(dp, NX), lax.rem(dp, NX)
    other = 1 - c
    partner = 2 * y + other
    label = lax.rem(x + 2 * z, 4)
    owner_lane, owner_slot = lax.div(sp, HALF), lax.rem(sp, HALF)
    x_up = z * NX + lax.rem(x + 1, NX)
    x_dn = z * NX + lax.rem(x + NX - 1, NX)
    z_up = lax.rem(z + 1, NZ) * NX + x
    z_dn = lax.rem(z + NZ - 1, NZ) * NX + x
    y_up = 2 * lax.rem(y + 1, NY) + c
    y_dn = 2 * lax.rem(y + NY - 1, NY) + c

    def remote(src, dst, send, recv, to_sp, to_dp):
        return pltpu.make_async_remote_copy(
            src_ref=src, dst_ref=dst, send_sem=send, recv_sem=recv,
            device_id=(to_sp, to_dp), device_id_type=MESH,
        )

    mine = pl.ds(pl.multiple_of(c * LANE, LANE), LANE)
    theirs = pl.ds(pl.multiple_of(other * LANE, LANE), LANE)
    my_rows = pl.ds(pl.multiple_of(c * TOK, TOK), TOK)
    sources = (k_ref, v_ref, q_ref, g_ref)

    row_load = pltpu.make_async_copy(ld_ref.at[0], row_buf, row_sem)
    row_load.start()
    loads = [
        pltpu.make_async_copy(ref.at[0, :, mine], x_buf.at[i, my_rows, :], load_sem.at[i])
        for i, ref in enumerate(sources)
    ]
    for copy in loads:
        copy.start()
    w_load = pltpu.make_async_copy(w_ref.at[mine, :], w_buf.at[sp], w_load_sem)
    w_load.start()

    barrier = pltpu.get_barrier_semaphore()

    def greet(step, carry):
        to = lax.rem(sp + step, 2 * NY)
        pl.semaphore_signal(barrier, inc=1, device_id=(to, dp), device_id_type=MESH)
        return carry

    lax.fori_loop(1, 2 * NY, greet, 0)
    for to in (x_up, x_dn, z_up, z_dn):
        pl.semaphore_signal(barrier, inc=1, device_id=(sp, to), device_id_type=MESH)

    lane_id = lax.broadcasted_iota(jnp.int32, (SPAN, SIZE), 1)
    place = lax.broadcasted_iota(jnp.int32, (SPAN, SIZE), 0) + y * SPAN
    freq = jnp.where(lane_id >= SIZE // 2, lane_id - SIZE // 2, lane_id).astype(F32)
    angle = place.astype(F32) * jnp.exp(freq * (-math.log(ROTARY_BASE) / (SIZE // 2)))
    cos_t[...] = jnp.cos(angle)
    sine = jnp.sin(angle)
    sin_t[...] = jnp.where(lane_id >= SIZE // 2, sine, -sine)

    pl.semaphore_wait(barrier, 2 * NY - 1 + 4)

    row_load.wait()

    def decay_copy(to_y):
        to = 2 * to_y + owner_lane
        at = pl.ds(pl.multiple_of(to_y * SPAN, SPAN), SPAN)
        return to, remote(
            row_buf.at[:, at], dec.at[owner_slot], ds_sem.at[to_y], dr_sem.at[owner_slot], to, dp
        )

    def decay_send(step, carry):
        to, copy = decay_copy(lax.rem(y + step, NY))

        @pl.when(to != sp)
        def _():
            copy.start()

        return carry

    lax.fori_loop(0, NY, decay_send, 0)

    @pl.when(owner_lane == c)
    def _():
        dec[owner_slot] = row_buf[:, pl.ds(pl.multiple_of(y * SPAN, SPAN), SPAN)]

    swaps = [
        remote(
            ref.at[0, :, theirs], x_buf.at[i, my_rows, :], xs_sem.at[i], xr_sem.at[i], partner, dp
        )
        for i, ref in enumerate(sources)
    ]
    w_swap = remote(w_ref.at[theirs, :], w_buf.at[sp], ws_sem, wr_sem, partner, dp)
    for copy in swaps[:2]:
        copy.start()
    w_swap.start()
    for copy in swaps[2:]:
        copy.start()

    def cols(j):
        return pl.ds(pl.multiple_of(j * SIZE, SIZE), SIZE)

    def turn(raw):
        return raw * cos_t[...] + pltpu.roll(raw, SIZE // 2, 1) * sin_t[...]

    def w_piece(block, start=0, size=PIECE):
        rows = pl.ds(pl.multiple_of(label * PIECE + start, 128), size)
        return w_buf.at[pl.ds(2 * block, 2), rows, :]

    def up_copy(s):
        block = lax.rem(y + NY - s, NY)
        return remote(w_piece(block), w_piece(block), ys_sem.at[s], yr_sem.at[s], y_up, dp)

    def dn_copy(s):
        block = lax.rem(y + s, NY)
        return remote(w_piece(block), w_piece(block), ys_sem.at[4 + s], yr_sem.at[4 + s], y_dn, dp)

    def spread_copies(slot, block):
        return (
            remote(w_piece(block), w_piece(block), ns_sem.at[0, slot], nr_sem.at[0, slot], sp, x_up),
            remote(w_piece(block), w_piece(block), ns_sem.at[1, slot], nr_sem.at[1, slot], sp, x_dn),
            remote(
                w_piece(block, 0, 128), w_piece(block, 0, 128),
                ns_sem.at[2, slot], nr_sem.at[2, slot], sp, z_up,
            ),
            remote(
                w_piece(block, 128, 128), w_piece(block, 128, 128),
                ns_sem.at[3, slot], nr_sem.at[3, slot], sp, z_dn,
            ),
        )

    def spread(slot, block):
        for copy in spread_copies(slot, block):
            copy.start()

    for copy in loads[:2]:
        copy.wait()
    for copy in swaps[:2]:
        copy.wait_recv()

    def turn_k(j, carry):
        krot[j] = turn(x_buf[0, :, cols(j)].astype(F32))
        return carry

    lax.fori_loop(0, HALF, turn_k, 0)

    w_load.wait()
    w_swap.wait_recv()
    up_copy(0).start()
    dn_copy(0).start()

    def decay_wait(j, carry):
        @pl.when(HALF * c + j != sp)
        def _():
            at = pl.ds(0, SPAN)
            remote(row_buf.at[:, at], dec.at[j], ds_sem.at[0], dr_sem.at[j], partner, dp).wait_recv()

        return carry

    lax.fori_loop(0, HALF, decay_wait, 0)

    up_rows = lax.broadcasted_iota(jnp.int32, (SPAN, SPAN), 0)
    up_cols = lax.broadcasted_iota(jnp.int32, (SPAN, SPAN), 1)
    causal = up_rows >= up_cols
    lower = jnp.where(causal, 1.0, 0.0).astype(F32)
    decays = jnp.concatenate([dec[j] for j in range(HALF)], axis=0)
    summed = exact(decays, lower, 1, 1)
    summed_t = exact(lower, decays, 1, 1)
    for j in range(HALF):
        sum_buf[j] = summed[j : j + 1, :]
        col_buf[j] = jnp.broadcast_to(summed_t[:, j : j + 1], (SPAN, SIZE))

    def g_copy(j):
        return remote(
            g_send.at[j], g_recv.at[y], gs_sem.at[j], gr_sem.at[y], HALF * c + j, dp
        )

    def grow(j, carry):
        col = col_buf[j]
        high, low = split(krot[j] * jnp.exp(col[SPAN - 1 :, :] - col))
        v = x_buf[1, :, cols(j)]
        piece = (dot(high, v, 0, 0) + dot(low, v, 0, 0)).astype(BF16)
        to = HALF * c + j

        @pl.when(to == sp)
        def _():
            g_recv[y] = piece

        @pl.when(jnp.logical_and(to != sp, y != NY - 1))
        def _():
            g_send[j] = piece
            g_copy(j).start()

        return carry

    lax.fori_loop(0, HALF, grow, 0)

    def ring_step(s):
        up_copy(s - 1).wait_recv()
        if s < 4:
            up_copy(s).start()
        if s < 4:
            dn_copy(s - 1).wait_recv()
            if s < 3:
                dn_copy(s).start()
        spread(s - 1, lax.rem(y + NY - s, NY))
        if s < 4:
            spread(3 + s, lax.rem(y + s, NY))

    for copy in loads[2:]:
        copy.wait()
    for copy in swaps[2:]:
        copy.wait_recv()

    def turn_q(j, carry):
        qrot[j] = turn(x_buf[2, :, cols(j)].astype(F32))
        return carry

    lax.fori_loop(0, HALF, turn_q, 0)
    ring_step(1)

    def attend(j, carry):
        qh, ql = split(qrot[j])
        kh, kl = split(krot[j])
        score = dot(qh, kh, 1, 1) + dot(qh, kl, 1, 1) + dot(ql, kh, 1, 1)
        col = col_buf[j]
        gap = jnp.concatenate([col, col], axis=1) - sum_buf[j]
        gap = jnp.where(causal, gap, -1e30)
        ph, plow = split(score * jnp.exp(gap))
        v = x_buf[1, :, cols(j)]
        inner[j] = dot(ph, v, 1, 0) + dot(plow, v, 1, 0)
        return carry

    lax.fori_loop(0, 4, attend, 0)
    ring_step(2)
    lax.fori_loop(4, HALF, attend, 0)
    ring_step(3)

    def s_copy(to_y):
        to = 2 * to_y + owner_lane
        return to, remote(
            s_send.at[to_y], s_recv.at[owner_slot], ss_sem.at[to_y], sr_sem.at[owner_slot], to, dp
        )

    state[...] = jnp.zeros_like(state)

    @pl.when(y == 0)
    def _():
        s_recv[...] = jnp.zeros_like(s_recv)

    def scan(src, carry):
        @pl.when(jnp.logical_not(jnp.logical_and(src == y, owner_lane == c)))
        def _():
            remote(
                g_send.at[0], g_recv.at[src], gs_sem.at[0], gr_sem.at[src], partner, dp
            ).wait_recv()

        at = pl.ds(pl.multiple_of(src * SPAN, SPAN), SPAN)
        fade = jnp.exp(jnp.sum(row_buf[:, at], axis=1, keepdims=True))
        new = state[...] * fade + g_recv[src].astype(F32)
        state[...] = new
        to, copy = s_copy(src + 1)

        @pl.when(to == sp)
        def _():
            s_recv[owner_slot] = new.astype(BF16)

        @pl.when(to != sp)
        def _():
            s_send[src + 1] = new.astype(BF16)
            copy.start()

        return carry

    lax.fori_loop(0, NY - 1, scan, 0)
    ring_step(4)

    def finish(j, carry):
        @pl.when(jnp.logical_and(y > 0, HALF * c + j != sp))
        def _():
            remote(
                s_send.at[0], s_recv.at[j], ss_sem.at[0], sr_sem.at[j], partner, dp
            ).wait_recv()

        qh, ql = split(qrot[j] * jnp.exp(col_buf[j]))
        entering = s_recv[j]
        result = inner[j] + dot(qh, entering, 1, 0) + dot(ql, entering, 1, 0)
        scale = lax.rsqrt(jnp.mean(result * result, axis=1, keepdims=True) + EPS)
        gate = x_buf[3, :, cols(j)].astype(F32)
        hidden[:, cols(j)] = (result * scale * (gate / (1.0 + jnp.exp(-gate)))).astype(BF16)
        return carry

    lax.fori_loop(0, HALF, finish, 0)

    def p_copy(block):
        return remote(
            p_send.at[block], p_recv.at[block], ps_sem.at[block], pr_sem.at[block], partner, dp
        )

    their_rows = pl.ds(pl.multiple_of(other * TOK, TOK), TOK)

    def project(block):
        rhs = jnp.concatenate([w_buf[2 * block], w_buf[2 * block + 1]], axis=1)
        p_send[block] = dot(hidden[their_rows, :], rhs, 1, 0)
        p_copy(block).start()
        p_own[block] = dot(hidden[my_rows, :], rhs, 1, 0)

    def project_far(slot, block):
        for copy in spread_copies(slot, block):
            copy.wait_recv()
        project(block)

    project(y)

    def project_down(s, carry):
        project_far(s - 1, lax.rem(y + NY - s, NY))
        return carry

    def project_up(s, carry):
        project_far(3 + s, lax.rem(y + s, NY))
        return carry

    lax.fori_loop(1, 5, project_down, 0)
    lax.fori_loop(1, 4, project_up, 0)

    def gather(block, carry):
        p_copy(block).wait_recv()
        at = pl.ds(pl.multiple_of(block * SPAN, SPAN), SPAN)
        out_ref[0, :, at] = (p_own[block] + p_recv[block]).astype(BF16)
        return carry

    lax.fori_loop(0, NY, gather, 0)

    for copy in swaps:
        copy.wait_send()
    w_swap.wait_send()

    def drain_decay(to_y, carry):
        to, copy = decay_copy(to_y)

        @pl.when(to != sp)
        def _():
            copy.wait_send()

        return carry

    def drain_g(j, carry):
        @pl.when(jnp.logical_and(HALF * c + j != sp, y != NY - 1))
        def _():
            g_copy(j).wait_send()

        return carry

    def drain_s(to_y, carry):
        to, copy = s_copy(to_y)

        @pl.when(to != sp)
        def _():
            copy.wait_send()

        return carry

    def drain_spread(slot, carry):
        for copy in spread_copies(slot, y):
            copy.wait_send()
        return carry

    def drain_p(block, carry):
        p_copy(block).wait_send()
        return carry

    lax.fori_loop(0, NY, drain_decay, 0)
    lax.fori_loop(0, HALF, drain_g, 0)
    lax.fori_loop(1, NY, drain_s, 0)
    for s in range(4):
        up_copy(s).wait_send()
    for s in range(3):
        dn_copy(s).wait_send()
    lax.fori_loop(0, NY - 1, drain_spread, 0)
    lax.fori_loop(0, NY, drain_p, 0)


def on_device(q, k, v, gates, log_decay, weight):
    dma = pltpu.SemaphoreType.DMA
    vmem = pltpu.VMEM
    state_shape = (NY, SIZE, SIZE)
    return pl.pallas_call(
        kernel,
        out_shape=jax.ShapeDtypeStruct(q.shape, BF16),
        in_specs=[pl.BlockSpec(memory_space=pl.ANY)] * 6,
        out_specs=pl.BlockSpec(memory_space=pltpu.VMEM),
        scratch_shapes=[
            vmem((4, SPAN, LANE), BF16),
            vmem((1, NY * SPAN), F32),
            vmem((HALF, 1, SPAN), F32),
            vmem((HEADS, LANE, SIZE), BF16),
            vmem((SPAN, SIZE), F32),
            vmem((SPAN, SIZE), F32),
            vmem((HALF, SPAN, SIZE), F32),
            vmem((HALF, 1, SPAN), F32),
            vmem((HALF, SPAN, SIZE), F32),
            vmem((HALF, SPAN, SIZE), F32),
            vmem((HALF, SPAN, SIZE), F32),
            vmem(state_shape, BF16),
            vmem(state_shape, BF16),
            vmem(state_shape, BF16),
            vmem(state_shape, BF16),
            vmem((SIZE, SIZE), F32),
            vmem((SPAN, LANE), BF16),
            vmem((NY, TOK, SPAN), F32),
            vmem((NY, TOK, SPAN), F32),
            vmem((NY, TOK, SPAN), F32),
            dma((4,)),
            dma,
            dma,
            dma((4,)),
            dma((4,)),
            dma((NY,)),
            dma((HALF,)),
            dma,
            dma,
            dma((8,)),
            dma((8,)),
            dma((4, NY - 1)),
            dma((4, NY - 1)),
            dma((HALF,)),
            dma((NY,)),
            dma((NY,)),
            dma((HALF,)),
            dma((NY,)),
            dma((NY,)),
        ],
        compiler_params=pltpu.CompilerParams(
            collective_id=0, has_side_effects=True, vmem_limit_bytes=48 * 1024 * 1024
        ),
        name="retention",
    )(q, k, v, gates, log_decay, weight)


def solution(mesh):
    placed = (P("dp", "sp", None),) * 5 + (P(None, "sp"),)
    return jax.shard_map(
        on_device, mesh=mesh, in_specs=placed, out_specs=P("dp", "sp", None), check_vma=False
    )
```

```python
import math

import jax
import jax.numpy as jnp
from jax import lax
from jax.experimental import pallas as pl
from jax.experimental.pallas import tpu as pltpu
from jax.sharding import PartitionSpec as P

EPS = 1e-06
ROTARY_BASE = 10000.0
MESH = pl.DeviceIdType.MESH
F32, BF16 = jnp.float32, jnp.bfloat16
NX, NZ, NY = 4, 12, 8
HEADS, SIZE, TOK, HALF = 16, 128, 128, 8
SPAN = 2 * TOK
LANE = HALF * SIZE
PIECE = LANE // 8


def split(x):
    high = x.astype(BF16)
    return high, (x - high.astype(F32)).astype(BF16)


def dot(a, b, ca, cb):
    return lax.dot_general(a, b, (((ca,), (cb,)), ((), ())), preferred_element_type=F32)


def kernel(
    q_ref, k_ref, v_ref, g_ref, ld_ref, w_ref, out_ref,
    x_buf, row_buf, dec, w_mine, w_buf, cos_t, sin_t, tri_buf, col_buf, sum_buf, fade_row, fade_buf,
    k_turned, inner, lift, gated, g_send, g_recv, s_send, s_recv, state, hidden, p_buf, p_send, p_recv,
    load_sem, w_load_sem, row_sem, xs_sem, xr_sem, ds_sem, dr_sem, ws_sem, wr_sem,
    fs_sem, ys_sem, yr_sem, ns_sem, nr_sem, gs_sem, gr_sem, ss_sem, sr_sem,
    ps_sem, pr_sem,
):
    sp = lax.axis_index("sp")
    dp = lax.axis_index("dp")
    y, c = lax.div(sp, 2), lax.rem(sp, 2)
    z, x = lax.div(dp, NX), lax.rem(dp, NX)
    other = 1 - c
    partner = 2 * y + other
    owner_lane, owner_slot = lax.div(sp, HALF), lax.rem(sp, HALF)
    x_up = z * NX + lax.rem(x + 1, NX)
    x_dn = z * NX + lax.rem(x + NX - 1, NX)
    z_up = lax.rem(z + 1, NZ) * NX + x
    z_dn = lax.rem(z + NZ - 1, NZ) * NX + x
    y_next = (lax.rem(y + 1, NY), lax.rem(y + NY - 1, NY))
    piece_row = (
        PIECE * lax.rem(x + 2 * z, 4),
        LANE // 2 + PIECE * lax.rem(z + 2 * x, 4),
    )

    def remote(src, dst, send, recv, to_sp, to_dp):
        return pltpu.make_async_remote_copy(
            src_ref=src, dst_ref=dst, send_sem=send, recv_sem=recv,
            device_id=(to_sp, to_dp), device_id_type=MESH,
        )

    mine = pl.ds(pl.multiple_of(c * LANE, LANE), LANE)
    theirs = pl.ds(pl.multiple_of(other * LANE, LANE), LANE)
    my_rows = pl.ds(pl.multiple_of(c * TOK, TOK), TOK)
    their_rows = pl.ds(pl.multiple_of(other * TOK, TOK), TOK)
    sources = (k_ref, v_ref, q_ref, g_ref)

    row_load = pltpu.make_async_copy(ld_ref.at[0], row_buf, row_sem)
    row_load.start()
    w_load = pltpu.make_async_copy(w_ref, w_mine, w_load_sem)
    w_load.start()
    loads = [
        pltpu.make_async_copy(ref.at[0, :, mine], x_buf.at[i, my_rows, :], load_sem.at[i])
        for i, ref in enumerate(sources)
    ]
    for copy in loads:
        copy.start()
    barrier = pltpu.get_barrier_semaphore()

    def greet(step, carry):
        to = lax.rem(sp + step, 2 * NY)
        pl.semaphore_signal(barrier, inc=1, device_id=(to, dp), device_id_type=MESH)
        return carry

    lax.fori_loop(1, 2 * NY, greet, 0)
    for to in (x_up, x_dn, z_up, z_dn):
        pl.semaphore_signal(barrier, inc=1, device_id=(sp, to), device_id_type=MESH)

    lane_id = lax.broadcasted_iota(jnp.int32, (SPAN, SIZE), 1)
    place = lax.broadcasted_iota(jnp.int32, (SPAN, SIZE), 0) + y * SPAN
    freq = jnp.where(lane_id >= SIZE // 2, lane_id - SIZE // 2, lane_id).astype(F32)
    angle = place.astype(F32) * jnp.exp(freq * (-math.log(ROTARY_BASE) / (SIZE // 2)))
    cos_t[...] = jnp.cos(angle)
    sine = jnp.sin(angle)
    sin_t[...] = jnp.where(lane_id >= SIZE // 2, sine, -sine)
    tri_rows = lax.broadcasted_iota(jnp.int32, (SPAN, SPAN), 0)
    tri_cols = lax.broadcasted_iota(jnp.int32, (SPAN, SPAN), 1)
    tri_buf[...] = jnp.where(tri_rows >= tri_cols, 1.0, 0.0).astype(BF16)

    pl.semaphore_wait(barrier, 2 * NY - 1 + 4)

    row_load.wait()

    def decay_copy(to_y):
        to = 2 * to_y + owner_lane
        at = pl.ds(pl.multiple_of(to_y * SPAN, SPAN), SPAN)
        return to, remote(
            row_buf.at[:, at], dec.at[owner_slot], ds_sem.at[to_y], dr_sem.at[owner_slot], to, dp
        )

    def decay_send(step, carry):
        to, copy = decay_copy(lax.rem(y + step, NY))

        @pl.when(to != sp)
        def _():
            copy.start()

        return carry

    lax.fori_loop(0, NY, decay_send, 0)

    @pl.when(owner_lane == c)
    def _():
        dec[owner_slot] = row_buf[:, pl.ds(pl.multiple_of(y * SPAN, SPAN), SPAN)]

    swaps = [
        remote(
            ref.at[0, :, theirs], x_buf.at[i, my_rows, :], xs_sem.at[i], xr_sem.at[i], partner, dp
        )
        for i, ref in enumerate(sources)
    ]
    for copy in swaps[:2]:
        copy.start()

    def first_copy(way, piece, lane):
        src_rows = pl.ds(pl.multiple_of(lane * LANE + piece_row[piece], PIECE), PIECE)
        dst_rows = pl.ds(pl.multiple_of(piece_row[piece], PIECE), PIECE)
        return remote(
            w_mine.at[src_rows, :], w_buf.at[sp, dst_rows, :],
            fs_sem.at[way, piece, lane], yr_sem.at[way, piece, c, 1], 2 * y_next[way] + lane, dp,
        )

    w_load.wait()
    for piece in range(2):
        for lane in range(2):
            for way in range(2):
                first_copy(way, piece, lane).start()

    for copy in swaps[2:]:
        copy.start()
    w_swap = remote(w_mine.at[theirs, :], w_buf.at[sp], ws_sem, wr_sem, partner, dp)
    w_swap.start()
    w_buf[sp] = w_mine[mine, :]

    def cols(j):
        return pl.ds(pl.multiple_of(j * SIZE, SIZE), SIZE)

    def turn(raw):
        return raw * cos_t[...] + pltpu.roll(raw, SIZE // 2, 1) * sin_t[...]

    def block_at(way, s):
        return lax.rem(y + NY - s, NY) if way == 0 else lax.rem(y + s, NY)

    def w_piece(block, piece, start=0, size=PIECE):
        rows = pl.ds(pl.multiple_of(piece_row[piece] + start, 64), size)
        return w_buf.at[pl.ds(2 * block, 2), rows, :]

    def hop_copy(way, piece, shard, s):
        rows = pl.ds(pl.multiple_of(piece_row[piece], PIECE), PIECE)
        ref = w_buf.at[2 * block_at(way, s - 1) + shard, rows, :]
        return remote(
            ref, ref, ys_sem.at[way, piece, shard, s], yr_sem.at[way, piece, shard, s],
            2 * y_next[way] + c, dp,
        )

    def spread_copies(piece, slot, block):
        whole = w_piece(block, piece)
        lower, upper = w_piece(block, piece, 0, PIECE // 2), w_piece(block, piece, PIECE // 2, PIECE // 2)
        refs = (whole, whole, lower, upper) if piece == 0 else (lower, upper, whole, whole)
        return [
            remote(ref, ref, ns_sem.at[piece, k, slot], nr_sem.at[piece, k, slot], sp, to)
            for k, (ref, to) in enumerate(zip(refs, (x_up, x_dn, z_up, z_dn)))
        ]

    def slot_of(way, s):
        return 6 if s == 4 else 3 * way + s - 1

    def ring_step(s):
        kept = [(p, w) for p in range(2) for w in range(2) if s < 4 or p == w]
        for piece, way in kept:
            for shard in range(2):
                hop_copy(way, piece, shard, s).wait_recv()
                if s < 3 or (s == 3 and piece == way):
                    hop_copy(way, piece, shard, s + 1).start()
        for piece, way in kept:
            for copy in spread_copies(piece, slot_of(way, s), block_at(way, s)):
                copy.start()

    for copy in loads[:2]:
        copy.wait()
    for copy in swaps[:2]:
        copy.wait_recv()

    def turn_k(i, carry):
        for t in range(2):
            j = 2 * i + t
            k_turned[j] = turn(x_buf[0, :, cols(j)].astype(F32)).T
        return carry

    lax.fori_loop(0, HALF // 2, turn_k, 0)
    ring_step(1)

    def decay_wait(j, carry):
        @pl.when(HALF * c + j != sp)
        def _():
            at = pl.ds(0, SPAN)
            remote(row_buf.at[:, at], dec.at[j], ds_sem.at[0], dr_sem.at[j], partner, dp).wait_recv()

        return carry

    lax.fori_loop(0, HALF, decay_wait, 0)

    decays = jnp.concatenate([dec[j] for j in range(HALF)], axis=0)
    first = decays.astype(BF16).astype(F32)
    second = (decays - first).astype(BF16).astype(F32)
    third = decays - first - second
    terms = jnp.concatenate([first, second, third], axis=0).astype(BF16)
    parts = dot(terms, tri_buf[...], 1, 1)
    summed = parts[:HALF] + parts[HALF : 2 * HALF] + parts[2 * HALF :]
    fading = jnp.exp(summed[:, SPAN - 1 :] - summed)
    for j in range(HALF):
        fade_row[j] = fading[j : j + 1, :]
        sum_buf[j] = summed[j : j + 1, :]

    def g_copy(j):
        return remote(
            g_send.at[j], g_recv.at[y], gs_sem.at[j], gr_sem.at[y], HALF * c + j, dp
        )

    def grow(i, carry):
        for t in range(4):
            j = 4 * i + t
            high, low = split(k_turned[j] * fade_row[j])
            v = x_buf[1, :, cols(j)]
            g_send[j] = (dot(high, v, 1, 0) + dot(low, v, 1, 0)).astype(BF16)
        for t in range(4):
            j = 4 * i + t
            to = HALF * c + j

            @pl.when(to == sp)
            def _(j=j):
                g_recv[y] = g_send[j]

            @pl.when(jnp.logical_and(to != sp, y != NY - 1))
            def _(j=j):
                g_copy(j).start()

        return carry

    lax.fori_loop(0, HALF // 4, grow, 0)
    ring_step(2)

    parts_t = dot(tri_buf[...], terms, 1, 1)
    summed_t = parts_t[:, :HALF] + parts_t[:, HALF : 2 * HALF] + parts_t[:, 2 * HALF :]
    for j in range(HALF):
        col_buf[j] = jnp.broadcast_to(summed_t[:, j : j + 1], (SPAN, SIZE))

    def fade_of(src, carry):
        at = pl.ds(pl.multiple_of(src * SPAN, SPAN), SPAN)
        total = jnp.exp(jnp.sum(row_buf[:, at], axis=1, keepdims=True))
        fade_buf[src] = jnp.broadcast_to(total, (1, SIZE))
        return carry

    lax.fori_loop(0, NY - 1, fade_of, 0)

    for copy in loads[2:]:
        copy.wait()
    for copy in swaps[2:]:
        copy.wait_recv()

    def attend(i, carry):
        for t in range(2):
            j = 2 * i + t
            kh, kl = split(k_turned[j])
            gate = x_buf[3, :, cols(j)].astype(F32)
            gated[j] = gate / (1.0 + jnp.exp(-gate))
            for half in range(2):
                rows = slice(half * TOK, half * TOK + TOK)
                width = TOK * (half + 1)
                raw = x_buf[2, rows, cols(j)].astype(F32)
                turned = raw * cos_t[rows, :] + pltpu.roll(raw, SIZE // 2, 1) * sin_t[rows, :]
                qh, ql = split(turned)
                near = kh[:, :width]
                score = dot(qh, near, 1, 0) + dot(ql, near, 1, 0) + dot(qh, kl[:, :width], 1, 0)
                col = col_buf[j, rows, :]
                lh, ll = split(turned * jnp.exp(col))
                lift[j, rows, :SIZE] = lh
                lift[j, rows, SIZE:] = ll
                wide = jnp.concatenate([col] * (half + 1), axis=1)
                gap = wide - sum_buf[j][:, :width]
                at = lax.broadcasted_iota(jnp.int32, (TOK, width), 0) + half * TOK
                past = at >= lax.broadcasted_iota(jnp.int32, (TOK, width), 1)
                ph, plow = split(score * jnp.exp(jnp.where(past, gap, -1e30)))
                v = x_buf[1, :width, cols(j)]
                inner[j, rows, :] = dot(ph, v, 1, 0) + dot(plow, v, 1, 0)
        return carry

    ring_step(3)
    lax.fori_loop(0, 2, attend, 0)
    ring_step(4)
    lax.fori_loop(2, 4, attend, 0)

    def s_copy(to_y):
        to = 2 * to_y + owner_lane
        return to, remote(
            s_send.at[to_y], s_recv.at[owner_slot], ss_sem.at[to_y], sr_sem.at[owner_slot], to, dp
        )

    state[...] = jnp.zeros_like(state)

    @pl.when(y == 0)
    def _():
        s_recv[...] = jnp.zeros_like(s_recv)

    def scan(src, carry):
        @pl.when(jnp.logical_not(jnp.logical_and(src == y, owner_lane == c)))
        def _():
            remote(
                g_send.at[0], g_recv.at[src], gs_sem.at[0], gr_sem.at[src], partner, dp
            ).wait_recv()

        new = state[...] * fade_buf[src] + g_recv[src].astype(F32)
        state[...] = new
        to, copy = s_copy(src + 1)

        @pl.when(to == sp)
        def _():
            s_recv[owner_slot] = new.astype(BF16)

        @pl.when(to != sp)
        def _():
            s_send[src + 1] = new.astype(BF16)
            copy.start()

        return carry

    lax.fori_loop(0, NY - 1, scan, 0)

    def finish(i, carry):
        for t in range(2):
            j = 2 * i + t

            @pl.when(jnp.logical_and(y > 0, HALF * c + j != sp))
            def _(j=j):
                remote(
                    s_send.at[0], s_recv.at[j], ss_sem.at[0], sr_sem.at[j], partner, dp
                ).wait_recv()

        for t in range(2):
            j = 2 * i + t
            entering = s_recv[j]
            result = inner[j] + dot(lift[j], jnp.concatenate([entering, entering], axis=0), 1, 0)
            scale = lax.rsqrt(jnp.mean(result * result, axis=1, keepdims=True) + EPS)
            hidden[:, cols(j)] = (result * scale * gated[j]).astype(BF16)
        return carry

    lax.fori_loop(0, HALF // 2, finish, 0)

    def p_copy(block):
        return remote(
            p_send.at[block], p_recv.at[block], ps_sem.at[block], pr_sem.at[block], partner, dp
        )

    def project(block):
        rhs = jnp.concatenate([w_buf[2 * block], w_buf[2 * block + 1]], axis=1)
        p_buf[block] = dot(hidden[...], rhs, 1, 0)
        p_send[block] = p_buf[block, their_rows, :].astype(BF16)
        p_copy(block).start()

    w_swap.wait_recv()
    project(y)

    def project_far(slot, carry):
        way, s = lax.div(slot, 3), lax.rem(slot, 3) + 1
        step = jnp.where(slot == 6, 4, jnp.where(way == 0, NY - s, s))
        block = lax.rem(y + step, NY)
        for piece in range(2):
            for copy in spread_copies(piece, slot, block):
                copy.wait_recv()
        project(block)
        return carry

    lax.fori_loop(0, NY - 1, project_far, 0)

    def gather(i, carry):
        for t in range(2):
            block = 2 * i + t
            p_copy(block).wait_recv()
            at = pl.ds(pl.multiple_of(block * SPAN, SPAN), SPAN)
            total = p_buf[block, my_rows, :] + p_recv[block].astype(F32)
            out_ref[0, :, at] = total.astype(BF16)
        return carry

    lax.fori_loop(0, NY // 2, gather, 0)

    for copy in swaps:
        copy.wait_send()
    w_swap.wait_send()

    def drain_decay(to_y, carry):
        to, copy = decay_copy(to_y)

        @pl.when(to != sp)
        def _():
            copy.wait_send()

        return carry

    def drain_g(j, carry):
        @pl.when(jnp.logical_and(HALF * c + j != sp, y != NY - 1))
        def _():
            g_copy(j).wait_send()

        return carry

    def drain_s(to_y, carry):
        to, copy = s_copy(to_y)

        @pl.when(to != sp)
        def _():
            copy.wait_send()

        return carry

    def drain_spread(slot, carry):
        for piece in range(2):
            for copy in spread_copies(piece, slot, y):
                copy.wait_send()
        return carry

    def drain_p(block, carry):
        p_copy(block).wait_send()
        return carry

    lax.fori_loop(0, NY, drain_decay, 0)
    lax.fori_loop(0, HALF, drain_g, 0)
    lax.fori_loop(1, NY, drain_s, 0)
    for piece in range(2):
        for way in range(2):
            for lane in range(2):
                first_copy(way, piece, lane).wait_send()
                for s in (2, 3, 4):
                    if s < 4 or piece == way:
                        hop_copy(way, piece, lane, s).wait_send()
    lax.fori_loop(0, NY - 1, drain_spread, 0)
    lax.fori_loop(0, NY, drain_p, 0)


def on_device(q, k, v, gates, log_decay, weight):
    dma = pltpu.SemaphoreType.DMA
    vmem = pltpu.VMEM
    state_shape = (NY, SIZE, SIZE)
    return pl.pallas_call(
        kernel,
        out_shape=pltpu.VMEM(q.shape, BF16),
        in_specs=[pl.BlockSpec(memory_space=pltpu.HBM)] * 6,
        out_specs=pl.BlockSpec(memory_space=pltpu.VMEM),
        scratch_shapes=[
            vmem((4, SPAN, LANE), BF16),
            vmem((1, NY * SPAN), F32),
            vmem((HALF, 1, SPAN), F32),
            vmem((2 * LANE, SIZE), BF16),
            vmem((HEADS, LANE, SIZE), BF16),
            vmem((SPAN, SIZE), F32),
            vmem((SPAN, SIZE), F32),
            vmem((SPAN, SPAN), BF16),
            vmem((HALF, SPAN, SIZE), F32),
            vmem((HALF, 1, SPAN), F32),
            vmem((HALF, 1, SPAN), F32),
            vmem((NY, 1, SIZE), F32),
            vmem((HALF, SIZE, SPAN), F32),
            vmem((HALF, SPAN, SIZE), F32),
            vmem((HALF, SPAN, SPAN), BF16),
            vmem((HALF, SPAN, SIZE), F32),
            vmem(state_shape, BF16),
            vmem(state_shape, BF16),
            vmem(state_shape, BF16),
            vmem(state_shape, BF16),
            vmem((SIZE, SIZE), F32),
            vmem((SPAN, LANE), BF16),
            vmem((NY, SPAN, SPAN), F32),
            vmem((NY, TOK, SPAN), BF16),
            vmem((NY, TOK, SPAN), BF16),
            dma((4,)),
            dma,
            dma,
            dma((4,)),
            dma((4,)),
            dma((NY,)),
            dma((HALF,)),
            dma,
            dma,
            dma((2, 2, 2)),
            dma((2, 2, 2, 5)),
            dma((2, 2, 2, 5)),
            dma((2, 4, NY - 1)),
            dma((2, 4, NY - 1)),
            dma((HALF,)),
            dma((NY,)),
            dma((NY,)),
            dma((HALF,)),
            dma((NY,)),
            dma((NY,)),
        ],
        compiler_params=pltpu.CompilerParams(
            collective_id=0, has_side_effects=True, vmem_limit_bytes=60 * 1024 * 1024
        ),
        name="retention",
    )(q, k, v, gates, log_decay, weight)


def solution(mesh):
    placed = (P("dp", "sp", None),) * 5 + (P(None, "sp"),)
    return jax.shard_map(
        on_device, mesh=mesh, in_specs=placed, out_specs=P("dp", "sp", None), check_vma=False
    )
```

```python
import math

import jax
import jax.numpy as jnp
from jax import lax
from jax.experimental import pallas as pl
from jax.experimental.pallas import tpu as pltpu
from jax.sharding import PartitionSpec as P

EPS = 1e-06
ROTARY_BASE = 10000.0
MESH = pl.DeviceIdType.MESH
F32, BF16 = jnp.float32, jnp.bfloat16
NX, NZ, NY = 4, 12, 8
HEADS, SIZE, TOK, HALF = 16, 128, 128, 8
SPAN = 2 * TOK
LANE = HALF * SIZE
PIECE = LANE // 8


def split(x):
    high = x.astype(BF16)
    return high, (x - high.astype(F32)).astype(BF16)


def dot(a, b, ca, cb):
    return lax.dot_general(a, b, (((ca,), (cb,)), ((), ())), preferred_element_type=F32)


def kernel(
    q_ref, k_ref, v_ref, g_ref, ld_ref, w_ref, out_ref,
    x_buf, row_buf, dec, w_mine, w_buf, cos_t, sin_t, tri_buf, col_buf, sum_buf, fade_row, fade_buf,
    k_turned, inner, lift, gated, g_send, g_recv, s_send, s_recv, state, hidden, p_buf, p_send, p_recv,
    load_sem, w_load_sem, row_sem, xs_sem, xr_sem, ds_sem, dr_sem, ws_sem, wr_sem,
    fs_sem, ys_sem, yr_sem, ns_sem, nr_sem, gs_sem, gr_sem, ss_sem, sr_sem,
    ps_sem, pr_sem,
):
    sp = lax.axis_index("sp")
    dp = lax.axis_index("dp")
    y, c = lax.div(sp, 2), lax.rem(sp, 2)
    z, x = lax.div(dp, NX), lax.rem(dp, NX)
    other = 1 - c
    partner = 2 * y + other
    owner_lane, owner_slot = lax.div(sp, HALF), lax.rem(sp, HALF)
    x_up = z * NX + lax.rem(x + 1, NX)
    x_dn = z * NX + lax.rem(x + NX - 1, NX)
    z_up = lax.rem(z + 1, NZ) * NX + x
    z_dn = lax.rem(z + NZ - 1, NZ) * NX + x
    y_next = (lax.rem(y + 1, NY), lax.rem(y + NY - 1, NY))
    piece_row = (
        PIECE * lax.rem(x + 2 * z, 4),
        LANE // 2 + PIECE * lax.rem(z + 2 * x, 4),
    )

    def remote(src, dst, send, recv, to_sp, to_dp):
        return pltpu.make_async_remote_copy(
            src_ref=src, dst_ref=dst, send_sem=send, recv_sem=recv,
            device_id=(to_sp, to_dp), device_id_type=MESH,
        )

    mine = pl.ds(pl.multiple_of(c * LANE, LANE), LANE)
    theirs = pl.ds(pl.multiple_of(other * LANE, LANE), LANE)
    my_rows = pl.ds(pl.multiple_of(c * TOK, TOK), TOK)
    their_rows = pl.ds(pl.multiple_of(other * TOK, TOK), TOK)
    sources = (k_ref, v_ref, q_ref, g_ref)

    row_load = pltpu.make_async_copy(ld_ref.at[0], row_buf, row_sem)
    row_load.start()
    w_load = pltpu.make_async_copy(w_ref, w_mine, w_load_sem)
    w_load.start()
    loads = [
        pltpu.make_async_copy(ref.at[0, :, mine], x_buf.at[i, my_rows, :], load_sem.at[i])
        for i, ref in enumerate(sources)
    ]
    for copy in loads:
        copy.start()
    barrier = pltpu.get_barrier_semaphore()

    def greet(step, carry):
        to = lax.rem(sp + step, 2 * NY)
        pl.semaphore_signal(barrier, inc=1, device_id=(to, dp), device_id_type=MESH)
        return carry

    lax.fori_loop(1, 2 * NY, greet, 0)
    for to in (x_up, x_dn, z_up, z_dn):
        pl.semaphore_signal(barrier, inc=1, device_id=(sp, to), device_id_type=MESH)

    lane_id = lax.broadcasted_iota(jnp.int32, (SPAN, SIZE), 1)
    place = lax.broadcasted_iota(jnp.int32, (SPAN, SIZE), 0) + y * SPAN
    freq = jnp.where(lane_id >= SIZE // 2, lane_id - SIZE // 2, lane_id).astype(F32)
    angle = place.astype(F32) * jnp.exp(freq * (-math.log(ROTARY_BASE) / (SIZE // 2)))
    cos_t[...] = jnp.cos(angle)
    sine = jnp.sin(angle)
    sin_t[...] = jnp.where(lane_id >= SIZE // 2, sine, -sine)
    tri_rows = lax.broadcasted_iota(jnp.int32, (SPAN, SPAN), 0)
    tri_cols = lax.broadcasted_iota(jnp.int32, (SPAN, SPAN), 1)
    tri_buf[...] = jnp.where(tri_rows >= tri_cols, 1.0, 0.0).astype(BF16)

    pl.semaphore_wait(barrier, 2 * NY - 1 + 4)

    row_load.wait()

    def decay_copy(to_y):
        to = 2 * to_y + owner_lane
        at = pl.ds(pl.multiple_of(to_y * SPAN, SPAN), SPAN)
        return to, remote(
            row_buf.at[:, at], dec.at[owner_slot], ds_sem.at[to_y], dr_sem.at[owner_slot], to, dp
        )

    def decay_send(step, carry):
        to, copy = decay_copy(lax.rem(y + step, NY))

        @pl.when(to != sp)
        def _():
            copy.start()

        return carry

    lax.fori_loop(0, NY, decay_send, 0)

    @pl.when(owner_lane == c)
    def _():
        dec[owner_slot] = row_buf[:, pl.ds(pl.multiple_of(y * SPAN, SPAN), SPAN)]

    swaps = [
        remote(
            ref.at[0, :, theirs], x_buf.at[i, my_rows, :], xs_sem.at[i], xr_sem.at[i], partner, dp
        )
        for i, ref in enumerate(sources)
    ]
    for copy in swaps[:2]:
        copy.start()

    def first_copy(way, piece, lane):
        src_rows = pl.ds(pl.multiple_of(lane * LANE + piece_row[piece], PIECE), PIECE)
        dst_rows = pl.ds(pl.multiple_of(piece_row[piece], PIECE), PIECE)
        return remote(
            w_mine.at[src_rows, :], w_buf.at[sp, dst_rows, :],
            fs_sem.at[way, piece, lane], yr_sem.at[way, piece, c, 1], 2 * y_next[way] + lane, dp,
        )

    w_load.wait()
    for piece in range(2):
        for lane in range(2):
            for way in range(2):
                first_copy(way, piece, lane).start()

    for copy in swaps[2:]:
        copy.start()
    w_swap = remote(w_mine.at[theirs, :], w_buf.at[sp], ws_sem, wr_sem, partner, dp)
    w_swap.start()
    w_buf[sp] = w_mine[mine, :]

    def cols(j):
        return pl.ds(pl.multiple_of(j * SIZE, SIZE), SIZE)

    def turn(raw):
        return raw * cos_t[...] + pltpu.roll(raw, SIZE // 2, 1) * sin_t[...]

    def block_at(way, s):
        return lax.rem(y + NY - s, NY) if way == 0 else lax.rem(y + s, NY)

    def w_piece(block, piece, start=0, size=PIECE):
        rows = pl.ds(pl.multiple_of(piece_row[piece] + start, 64), size)
        return w_buf.at[pl.ds(2 * block, 2), rows, :]

    def hop_copy(way, piece, shard, s):
        rows = pl.ds(pl.multiple_of(piece_row[piece], PIECE), PIECE)
        ref = w_buf.at[2 * block_at(way, s - 1) + shard, rows, :]
        return remote(
            ref, ref, ys_sem.at[way, piece, shard, s], yr_sem.at[way, piece, shard, s],
            2 * y_next[way] + c, dp,
        )

    def spread_copies(piece, slot, block):
        whole = w_piece(block, piece)
        lower, upper = w_piece(block, piece, 0, PIECE // 2), w_piece(block, piece, PIECE // 2, PIECE // 2)
        refs = (whole, whole, lower, upper) if piece == 0 else (lower, upper, whole, whole)
        return [
            remote(ref, ref, ns_sem.at[piece, k, slot], nr_sem.at[piece, k, slot], sp, to)
            for k, (ref, to) in enumerate(zip(refs, (x_up, x_dn, z_up, z_dn)))
        ]

    def slot_of(way, s):
        return 6 if s == 4 else 3 * way + s - 1

    def ring_step(s):
        kept = [(p, w) for p in range(2) for w in range(2) if s < 4 or p == w]
        for piece, way in kept:
            for shard in range(2):
                hop_copy(way, piece, shard, s).wait_recv()
                if s < 3 or (s == 3 and piece == way):
                    hop_copy(way, piece, shard, s + 1).start()
        for piece, way in kept:
            for copy in spread_copies(piece, slot_of(way, s), block_at(way, s)):
                copy.start()

    for copy in loads[:2]:
        copy.wait()
    for copy in swaps[:2]:
        copy.wait_recv()

    def turn_k(i, carry):
        for t in range(2):
            j = 2 * i + t
            k_turned[j] = turn(x_buf[0, :, cols(j)].astype(F32)).T
        return carry

    lax.fori_loop(0, HALF // 2, turn_k, 0)
    ring_step(1)

    def decay_wait(j, carry):
        @pl.when(HALF * c + j != sp)
        def _():
            at = pl.ds(0, SPAN)
            remote(row_buf.at[:, at], dec.at[j], ds_sem.at[0], dr_sem.at[j], partner, dp).wait_recv()

        return carry

    lax.fori_loop(0, HALF, decay_wait, 0)

    decays = jnp.concatenate([dec[j] for j in range(HALF)], axis=0)
    first = decays.astype(BF16).astype(F32)
    second = (decays - first).astype(BF16).astype(F32)
    third = decays - first - second
    terms = jnp.concatenate([first, second, third], axis=0).astype(BF16)
    parts = dot(terms, tri_buf[...], 1, 1)
    summed = parts[:HALF] + parts[HALF : 2 * HALF] + parts[2 * HALF :]
    fading = jnp.exp(summed[:, SPAN - 1 :] - summed)
    for j in range(HALF):
        fade_row[j] = fading[j : j + 1, :]
        sum_buf[j] = summed[j : j + 1, :]

    def g_copy(j):
        return remote(
            g_send.at[j], g_recv.at[y], gs_sem.at[j], gr_sem.at[y], HALF * c + j, dp
        )

    def grow(i, carry):
        for t in range(4):
            j = 4 * i + t
            high, low = split(k_turned[j] * fade_row[j])
            v = x_buf[1, :, cols(j)]
            g_send[j] = (dot(high, v, 1, 0) + dot(low, v, 1, 0)).astype(BF16)
        for t in range(4):
            j = 4 * i + t
            to = HALF * c + j

            @pl.when(to == sp)
            def _(j=j):
                g_recv[y] = g_send[j]

            @pl.when(jnp.logical_and(to != sp, y != NY - 1))
            def _(j=j):
                g_copy(j).start()

        return carry

    lax.fori_loop(0, HALF // 4, grow, 0)
    ring_step(2)

    parts_t = dot(tri_buf[...], terms, 1, 1)
    summed_t = parts_t[:, :HALF] + parts_t[:, HALF : 2 * HALF] + parts_t[:, 2 * HALF :]
    for j in range(HALF):
        col_buf[j] = jnp.broadcast_to(summed_t[:, j : j + 1], (SPAN, SIZE))

    def fade_of(src, carry):
        at = pl.ds(pl.multiple_of(src * SPAN, SPAN), SPAN)
        total = jnp.exp(jnp.sum(row_buf[:, at], axis=1, keepdims=True))
        fade_buf[src] = jnp.broadcast_to(total, (1, SIZE))
        return carry

    lax.fori_loop(0, NY - 1, fade_of, 0)

    for copy in loads[2:]:
        copy.wait()
    for copy in swaps[2:]:
        copy.wait_recv()

    def attend(i, carry):
        for t in range(2):
            j = 2 * i + t
            kh, kl = split(k_turned[j])
            gate = x_buf[3, :, cols(j)].astype(F32)
            gated[j] = gate / (1.0 + jnp.exp(-gate))
            for half in range(2):
                rows = slice(half * TOK, half * TOK + TOK)
                width = TOK * (half + 1)
                raw = x_buf[2, rows, cols(j)].astype(F32)
                turned = raw * cos_t[rows, :] + pltpu.roll(raw, SIZE // 2, 1) * sin_t[rows, :]
                qh, ql = split(turned)
                near = kh[:, :width]
                score = dot(qh, near, 1, 0) + dot(ql, near, 1, 0) + dot(qh, kl[:, :width], 1, 0)
                col = col_buf[j, rows, :]
                lh, ll = split(turned * jnp.exp(col))
                lift[j, rows, :SIZE] = lh
                lift[j, rows, SIZE:] = ll
                wide = jnp.concatenate([col] * (half + 1), axis=1)
                gap = wide - sum_buf[j][:, :width]
                at = lax.broadcasted_iota(jnp.int32, (TOK, width), 0) + half * TOK
                past = at >= lax.broadcasted_iota(jnp.int32, (TOK, width), 1)
                ph, plow = split(score * jnp.exp(jnp.where(past, gap, -1e30)))
                v = x_buf[1, :width, cols(j)]
                inner[j, rows, :] = dot(ph, v, 1, 0) + dot(plow, v, 1, 0)
        return carry

    lax.fori_loop(0, 2, attend, 0)
    lax.fori_loop(2, 4, attend, 0)
    ring_step(3)

    def s_copy(to_y):
        to = 2 * to_y + owner_lane
        return to, remote(
            s_send.at[to_y], s_recv.at[owner_slot], ss_sem.at[to_y], sr_sem.at[owner_slot], to, dp
        )

    state[...] = jnp.zeros_like(state)

    @pl.when(y == 0)
    def _():
        s_recv[...] = jnp.zeros_like(s_recv)

    def scan(src, carry):
        @pl.when(jnp.logical_not(jnp.logical_and(src == y, owner_lane == c)))
        def _():
            remote(
                g_send.at[0], g_recv.at[src], gs_sem.at[0], gr_sem.at[src], partner, dp
            ).wait_recv()

        new = state[...] * fade_buf[src] + g_recv[src].astype(F32)
        state[...] = new
        to, copy = s_copy(src + 1)

        @pl.when(to == sp)
        def _():
            s_recv[owner_slot] = new.astype(BF16)

        @pl.when(to != sp)
        def _():
            s_send[src + 1] = new.astype(BF16)
            copy.start()

        return carry

    lax.fori_loop(0, NY - 1, scan, 0)
    ring_step(4)

    def finish(i, carry):
        for t in range(2):
            j = 2 * i + t

            @pl.when(jnp.logical_and(y > 0, HALF * c + j != sp))
            def _(j=j):
                remote(
                    s_send.at[0], s_recv.at[j], ss_sem.at[0], sr_sem.at[j], partner, dp
                ).wait_recv()

        for t in range(2):
            j = 2 * i + t
            entering = s_recv[j]
            result = inner[j] + dot(lift[j], jnp.concatenate([entering, entering], axis=0), 1, 0)
            scale = lax.rsqrt(jnp.mean(result * result, axis=1, keepdims=True) + EPS)
            hidden[:, cols(j)] = (result * scale * gated[j]).astype(BF16)
        return carry

    lax.fori_loop(0, HALF // 2, finish, 0)

    def p_copy(block):
        return remote(
            p_send.at[block], p_recv.at[block], ps_sem.at[block], pr_sem.at[block], partner, dp
        )

    def project(block):
        rhs = jnp.concatenate([w_buf[2 * block], w_buf[2 * block + 1]], axis=1)
        p_buf[block] = dot(hidden[...], rhs, 1, 0)
        p_send[block] = p_buf[block, their_rows, :].astype(BF16)
        p_copy(block).start()

    w_swap.wait_recv()
    project(y)

    def project_far(slot, carry):
        way, s = lax.div(slot, 3), lax.rem(slot, 3) + 1
        step = jnp.where(slot == 6, 4, jnp.where(way == 0, NY - s, s))
        block = lax.rem(y + step, NY)
        for piece in range(2):
            for copy in spread_copies(piece, slot, block):
                copy.wait_recv()
        project(block)
        return carry

    lax.fori_loop(0, NY - 1, project_far, 0)

    def gather(i, carry):
        for t in range(2):
            block = 2 * i + t
            p_copy(block).wait_recv()
            at = pl.ds(pl.multiple_of(block * SPAN, SPAN), SPAN)
            total = p_buf[block, my_rows, :] + p_recv[block].astype(F32)
            out_ref[0, :, at] = total.astype(BF16)
        return carry

    lax.fori_loop(0, NY // 2, gather, 0)

    for copy in swaps:
        copy.wait_send()
    w_swap.wait_send()

    def drain_decay(to_y, carry):
        to, copy = decay_copy(to_y)

        @pl.when(to != sp)
        def _():
            copy.wait_send()

        return carry

    def drain_g(j, carry):
        @pl.when(jnp.logical_and(HALF * c + j != sp, y != NY - 1))
        def _():
            g_copy(j).wait_send()

        return carry

    def drain_s(to_y, carry):
        to, copy = s_copy(to_y)

        @pl.when(to != sp)
        def _():
            copy.wait_send()

        return carry

    def drain_spread(slot, carry):
        for piece in range(2):
            for copy in spread_copies(piece, slot, y):
                copy.wait_send()
        return carry

    def drain_p(block, carry):
        p_copy(block).wait_send()
        return carry

    lax.fori_loop(0, NY, drain_decay, 0)
    lax.fori_loop(0, HALF, drain_g, 0)
    lax.fori_loop(1, NY, drain_s, 0)
    for piece in range(2):
        for way in range(2):
            for lane in range(2):
                first_copy(way, piece, lane).wait_send()
                for s in (2, 3, 4):
                    if s < 4 or piece == way:
                        hop_copy(way, piece, lane, s).wait_send()
    lax.fori_loop(0, NY - 1, drain_spread, 0)
    lax.fori_loop(0, NY, drain_p, 0)


def on_device(q, k, v, gates, log_decay, weight):
    dma = pltpu.SemaphoreType.DMA
    vmem = pltpu.VMEM
    state_shape = (NY, SIZE, SIZE)
    return pl.pallas_call(
        kernel,
        out_shape=pltpu.VMEM(q.shape, BF16),
        in_specs=[pl.BlockSpec(memory_space=pltpu.HBM)] * 6,
        out_specs=pl.BlockSpec(memory_space=pltpu.VMEM),
        scratch_shapes=[
            vmem((4, SPAN, LANE), BF16),
            vmem((1, NY * SPAN), F32),
            vmem((HALF, 1, SPAN), F32),
            vmem((2 * LANE, SIZE), BF16),
            vmem((HEADS, LANE, SIZE), BF16),
            vmem((SPAN, SIZE), F32),
            vmem((SPAN, SIZE), F32),
            vmem((SPAN, SPAN), BF16),
            vmem((HALF, SPAN, SIZE), F32),
            vmem((HALF, 1, SPAN), F32),
            vmem((HALF, 1, SPAN), F32),
            vmem((NY, 1, SIZE), F32),
            vmem((HALF, SIZE, SPAN), F32),
            vmem((HALF, SPAN, SIZE), F32),
            vmem((HALF, SPAN, SPAN), BF16),
            vmem((HALF, SPAN, SIZE), F32),
            vmem(state_shape, BF16),
            vmem(state_shape, BF16),
            vmem(state_shape, BF16),
            vmem(state_shape, BF16),
            vmem((SIZE, SIZE), F32),
            vmem((SPAN, LANE), BF16),
            vmem((NY, SPAN, SPAN), F32),
            vmem((NY, TOK, SPAN), BF16),
            vmem((NY, TOK, SPAN), BF16),
            dma((4,)),
            dma,
            dma,
            dma((4,)),
            dma((4,)),
            dma((NY,)),
            dma((HALF,)),
            dma,
            dma,
            dma((2, 2, 2)),
            dma((2, 2, 2, 5)),
            dma((2, 2, 2, 5)),
            dma((2, 4, NY - 1)),
            dma((2, 4, NY - 1)),
            dma((HALF,)),
            dma((NY,)),
            dma((NY,)),
            dma((HALF,)),
            dma((NY,)),
            dma((NY,)),
        ],
        compiler_params=pltpu.CompilerParams(
            collective_id=0, has_side_effects=True, vmem_limit_bytes=60 * 1024 * 1024
        ),
        name="retention",
    )(q, k, v, gates, log_decay, weight)


def solution(mesh):
    placed = (P("dp", "sp", None),) * 5 + (P(None, "sp"),)
    return jax.shard_map(
        on_device, mesh=mesh, in_specs=placed, out_specs=P("dp", "sp", None), check_vma=False
    )
```

```python
import math

import jax
import jax.numpy as jnp
from jax import lax
from jax.experimental import pallas as pl
from jax.experimental.pallas import tpu as pltpu
from jax.sharding import PartitionSpec as P

EPS = 1e-06
ROTARY_BASE = 10000.0
MESH = pl.DeviceIdType.MESH
F32, BF16 = jnp.float32, jnp.bfloat16
NX, NZ, NY = 4, 12, 8
HEADS, SIZE, TOK, HALF = 16, 128, 128, 8
SPAN = 2 * TOK
LANE = HALF * SIZE
PIECE = LANE // 8


def split(x):
    high = x.astype(BF16)
    return high, (x - high.astype(F32)).astype(BF16)


def dot(a, b, ca, cb):
    return lax.dot_general(a, b, (((ca,), (cb,)), ((), ())), preferred_element_type=F32)


def kernel(
    q_ref, k_ref, v_ref, g_ref, ld_ref, w_ref, out_ref,
    x_buf, row_buf, dec, w_mine, w_buf, cos_t, sin_t, tri_buf, col_buf, sum_buf, fade_row, fade_buf,
    k_turned, inner, lift, gated, g_send, g_recv, s_send, s_recv, state, hidden, p_buf, p_send, p_recv,
    load_sem, w_load_sem, row_sem, xs_sem, xr_sem, ds_sem, dr_sem, ws_sem, wr_sem,
    fs_sem, ys_sem, yr_sem, ns_sem, nr_sem, gs_sem, gr_sem, ss_sem, sr_sem,
    ps_sem, pr_sem,
):
    sp = lax.axis_index("sp")
    dp = lax.axis_index("dp")
    y, c = lax.div(sp, 2), lax.rem(sp, 2)
    z, x = lax.div(dp, NX), lax.rem(dp, NX)
    other = 1 - c
    partner = 2 * y + other
    owner_lane, owner_slot = lax.div(sp, HALF), lax.rem(sp, HALF)
    x_up = z * NX + lax.rem(x + 1, NX)
    x_dn = z * NX + lax.rem(x + NX - 1, NX)
    z_up = lax.rem(z + 1, NZ) * NX + x
    z_dn = lax.rem(z + NZ - 1, NZ) * NX + x
    y_next = (lax.rem(y + 1, NY), lax.rem(y + NY - 1, NY))
    piece_row = (
        PIECE * lax.rem(x + 2 * z, 4),
        LANE // 2 + PIECE * lax.rem(z + 2 * x, 4),
    )

    def remote(src, dst, send, recv, to_sp, to_dp):
        return pltpu.make_async_remote_copy(
            src_ref=src, dst_ref=dst, send_sem=send, recv_sem=recv,
            device_id=(to_sp, to_dp), device_id_type=MESH,
        )

    mine = pl.ds(pl.multiple_of(c * LANE, LANE), LANE)
    theirs = pl.ds(pl.multiple_of(other * LANE, LANE), LANE)
    my_rows = pl.ds(pl.multiple_of(c * TOK, TOK), TOK)
    their_rows = pl.ds(pl.multiple_of(other * TOK, TOK), TOK)
    sources = (k_ref, v_ref, q_ref, g_ref)

    row_load = pltpu.make_async_copy(ld_ref.at[0], row_buf, row_sem)
    row_load.start()
    w_load = pltpu.make_async_copy(w_ref, w_mine, w_load_sem)
    w_load.start()
    loads = [
        pltpu.make_async_copy(ref.at[0, :, mine], x_buf.at[i, my_rows, :], load_sem.at[i])
        for i, ref in enumerate(sources)
    ]
    for copy in loads:
        copy.start()
    barrier = pltpu.get_barrier_semaphore()

    def greet(step, carry):
        to = lax.rem(sp + step, 2 * NY)
        pl.semaphore_signal(barrier, inc=1, device_id=(to, dp), device_id_type=MESH)
        return carry

    lax.fori_loop(1, 2 * NY, greet, 0)
    for to in (x_up, x_dn, z_up, z_dn):
        pl.semaphore_signal(barrier, inc=1, device_id=(sp, to), device_id_type=MESH)

    lane_id = lax.broadcasted_iota(jnp.int32, (SPAN, SIZE), 1)
    place = lax.broadcasted_iota(jnp.int32, (SPAN, SIZE), 0) + y * SPAN
    freq = jnp.where(lane_id >= SIZE // 2, lane_id - SIZE // 2, lane_id).astype(F32)
    angle = place.astype(F32) * jnp.exp(freq * (-math.log(ROTARY_BASE) / (SIZE // 2)))
    cos_t[...] = jnp.cos(angle)
    sine = jnp.sin(angle)
    sin_t[...] = jnp.where(lane_id >= SIZE // 2, sine, -sine)
    tri_rows = lax.broadcasted_iota(jnp.int32, (SPAN, SPAN), 0)
    tri_cols = lax.broadcasted_iota(jnp.int32, (SPAN, SPAN), 1)
    tri_buf[...] = jnp.where(tri_rows >= tri_cols, 1.0, 0.0).astype(BF16)

    pl.semaphore_wait(barrier, 2 * NY - 1 + 4)

    swaps = [
        remote(
            ref.at[0, :, theirs], x_buf.at[i, my_rows, :], xs_sem.at[i], xr_sem.at[i], partner, dp
        )
        for i, ref in enumerate(sources)
    ]
    for copy in swaps[:2]:
        copy.start()

    row_load.wait()

    def decay_copy(to_y):
        to = 2 * to_y + owner_lane
        at = pl.ds(pl.multiple_of(to_y * SPAN, SPAN), SPAN)
        return to, remote(
            row_buf.at[:, at], dec.at[owner_slot], ds_sem.at[to_y], dr_sem.at[owner_slot], to, dp
        )

    def decay_send(step, carry):
        to, copy = decay_copy(lax.rem(y + step, NY))

        @pl.when(to != sp)
        def _():
            copy.start()

        return carry

    lax.fori_loop(0, NY, decay_send, 0)

    @pl.when(owner_lane == c)
    def _():
        dec[owner_slot] = row_buf[:, pl.ds(pl.multiple_of(y * SPAN, SPAN), SPAN)]

    def first_copy(way, piece, lane):
        src_rows = pl.ds(pl.multiple_of(lane * LANE + piece_row[piece], PIECE), PIECE)
        dst_rows = pl.ds(pl.multiple_of(piece_row[piece], PIECE), PIECE)
        return remote(
            w_mine.at[src_rows, :], w_buf.at[sp, dst_rows, :],
            fs_sem.at[way, piece, lane], yr_sem.at[way, piece, c, 1], 2 * y_next[way] + lane, dp,
        )

    w_load.wait()
    for piece in range(2):
        for lane in range(2):
            for way in range(2):
                first_copy(way, piece, lane).start()

    for copy in swaps[2:]:
        copy.start()
    w_swap = remote(w_mine.at[theirs, :], w_buf.at[sp], ws_sem, wr_sem, partner, dp)
    w_swap.start()
    w_buf[sp] = w_mine[mine, :]

    def cols(j):
        return pl.ds(pl.multiple_of(j * SIZE, SIZE), SIZE)

    def turn(raw):
        return raw * cos_t[...] + pltpu.roll(raw, SIZE // 2, 1) * sin_t[...]

    def block_at(way, s):
        return lax.rem(y + NY - s, NY) if way == 0 else lax.rem(y + s, NY)

    def w_piece(block, piece, start=0, size=PIECE):
        rows = pl.ds(pl.multiple_of(piece_row[piece] + start, 64), size)
        return w_buf.at[pl.ds(2 * block, 2), rows, :]

    def hop_copy(way, piece, shard, s):
        rows = pl.ds(pl.multiple_of(piece_row[piece], PIECE), PIECE)
        ref = w_buf.at[2 * block_at(way, s - 1) + shard, rows, :]
        return remote(
            ref, ref, ys_sem.at[way, piece, shard, s], yr_sem.at[way, piece, shard, s],
            2 * y_next[way] + c, dp,
        )

    def spread_copies(piece, slot, block):
        whole = w_piece(block, piece)
        lower, upper = w_piece(block, piece, 0, PIECE // 2), w_piece(block, piece, PIECE // 2, PIECE // 2)
        refs = (whole, whole, lower, upper) if piece == 0 else (lower, upper, whole, whole)
        return [
            remote(ref, ref, ns_sem.at[piece, k, slot], nr_sem.at[piece, k, slot], sp, to)
            for k, (ref, to) in enumerate(zip(refs, (x_up, x_dn, z_up, z_dn)))
        ]

    def slot_of(way, s):
        return 6 if s == 4 else 3 * way + s - 1

    def ring_step(s):
        kept = [(p, w) for p in range(2) for w in range(2) if s < 4 or p == w]
        for piece, way in kept:
            for shard in range(2):
                hop_copy(way, piece, shard, s).wait_recv()
                if s < 3 or (s == 3 and piece == way):
                    hop_copy(way, piece, shard, s + 1).start()
        for piece, way in kept:
            for copy in spread_copies(piece, slot_of(way, s), block_at(way, s)):
                copy.start()

    for copy in loads[:2]:
        copy.wait()
    for copy in swaps[:2]:
        copy.wait_recv()

    def turn_k(i, carry):
        for t in range(2):
            j = 2 * i + t
            k_turned[j] = turn(x_buf[0, :, cols(j)].astype(F32)).T
        return carry

    lax.fori_loop(0, HALF // 2, turn_k, 0)
    ring_step(1)

    def decay_wait(j, carry):
        @pl.when(HALF * c + j != sp)
        def _():
            at = pl.ds(0, SPAN)
            remote(row_buf.at[:, at], dec.at[j], ds_sem.at[0], dr_sem.at[j], partner, dp).wait_recv()

        return carry

    lax.fori_loop(0, HALF, decay_wait, 0)

    decays = jnp.concatenate([dec[j] for j in range(HALF)], axis=0)
    first = decays.astype(BF16).astype(F32)
    second = (decays - first).astype(BF16).astype(F32)
    third = decays - first - second
    terms = jnp.concatenate([first, second, third], axis=0).astype(BF16)
    parts = dot(terms, tri_buf[...], 1, 1)
    summed = parts[:HALF] + parts[HALF : 2 * HALF] + parts[2 * HALF :]
    fading = jnp.exp(summed[:, SPAN - 1 :] - summed)
    for j in range(HALF):
        fade_row[j] = fading[j : j + 1, :]
        sum_buf[j] = summed[j : j + 1, :]

    def g_copy(j):
        return remote(
            g_send.at[j], g_recv.at[y], gs_sem.at[j], gr_sem.at[y], HALF * c + j, dp
        )

    def grow(i, carry):
        for t in range(4):
            j = 4 * i + t
            high, low = split(k_turned[j] * fade_row[j])
            v = x_buf[1, :, cols(j)]
            g_send[j] = (dot(high, v, 1, 0) + dot(low, v, 1, 0)).astype(BF16)
        for t in range(4):
            j = 4 * i + t
            to = HALF * c + j

            @pl.when(to == sp)
            def _(j=j):
                g_recv[y] = g_send[j]

            @pl.when(jnp.logical_and(to != sp, y != NY - 1))
            def _(j=j):
                g_copy(j).start()

        return carry

    lax.fori_loop(0, HALF // 4, grow, 0)

    def attend(i, carry):
        for t in range(2):
            j = 2 * i + t
            kh, kl = split(k_turned[j])
            gate = x_buf[3, :, cols(j)].astype(F32)
            gated[j] = gate / (1.0 + jnp.exp(-gate))
            for half in range(2):
                rows = slice(half * TOK, half * TOK + TOK)
                width = TOK * (half + 1)
                raw = x_buf[2, rows, cols(j)].astype(F32)
                turned = raw * cos_t[rows, :] + pltpu.roll(raw, SIZE // 2, 1) * sin_t[rows, :]
                qh, ql = split(turned)
                near = kh[:, :width]
                score = dot(qh, near, 1, 0) + dot(ql, near, 1, 0) + dot(qh, kl[:, :width], 1, 0)
                col = col_buf[j, rows, :]
                lh, ll = split(turned * jnp.exp(col))
                lift[j, rows, :SIZE] = lh
                lift[j, rows, SIZE:] = ll
                wide = jnp.concatenate([col] * (half + 1), axis=1)
                gap = wide - sum_buf[j][:, :width]
                at = lax.broadcasted_iota(jnp.int32, (TOK, width), 0) + half * TOK
                past = at >= lax.broadcasted_iota(jnp.int32, (TOK, width), 1)
                ph, plow = split(score * jnp.exp(jnp.where(past, gap, -1e30)))
                v = x_buf[1, :width, cols(j)]
                inner[j, rows, :] = dot(ph, v, 1, 0) + dot(plow, v, 1, 0)
        return carry


    def s_copy(to_y):
        to = 2 * to_y + owner_lane
        return to, remote(
            s_send.at[to_y], s_recv.at[owner_slot], ss_sem.at[to_y], sr_sem.at[owner_slot], to, dp
        )

    state[...] = jnp.zeros_like(state)

    @pl.when(y == 0)
    def _():
        s_recv[...] = jnp.zeros_like(s_recv)

    def scan(src, carry):
        @pl.when(jnp.logical_not(jnp.logical_and(src == y, owner_lane == c)))
        def _():
            remote(
                g_send.at[0], g_recv.at[src], gs_sem.at[0], gr_sem.at[src], partner, dp
            ).wait_recv()

        new = state[...] * fade_buf[src] + g_recv[src].astype(F32)
        state[...] = new
        to, copy = s_copy(src + 1)

        @pl.when(to == sp)
        def _():
            s_recv[owner_slot] = new.astype(BF16)

        @pl.when(to != sp)
        def _():
            s_send[src + 1] = new.astype(BF16)
            copy.start()

        return carry

    parts_t = dot(tri_buf[...], terms, 1, 1)
    summed_t = parts_t[:, :HALF] + parts_t[:, HALF : 2 * HALF] + parts_t[:, 2 * HALF :]
    for j in range(HALF):
        col_buf[j] = jnp.broadcast_to(summed_t[:, j : j + 1], (SPAN, SIZE))

    def fade_of(src, carry):
        at = pl.ds(pl.multiple_of(src * SPAN, SPAN), SPAN)
        total = jnp.exp(jnp.sum(row_buf[:, at], axis=1, keepdims=True))
        fade_buf[src] = jnp.broadcast_to(total, (1, SIZE))
        return carry

    lax.fori_loop(0, NY - 1, fade_of, 0)

    ring_step(2)
    for copy in loads[2:]:
        copy.wait()
    for copy in swaps[2:]:
        copy.wait_recv()

    lax.fori_loop(0, 2, attend, 0)
    ring_step(3)
    lax.fori_loop(0, NY - 1, scan, 0)
    lax.fori_loop(2, 4, attend, 0)
    ring_step(4)

    def finish(i, carry):
        for t in range(4):
            j = 4 * i + t

            @pl.when(jnp.logical_and(y > 0, HALF * c + j != sp))
            def _(j=j):
                remote(
                    s_send.at[0], s_recv.at[j], ss_sem.at[0], sr_sem.at[j], partner, dp
                ).wait_recv()

        for t in range(4):
            j = 4 * i + t
            entering = s_recv[j]
            result = inner[j] + dot(lift[j], jnp.concatenate([entering, entering], axis=0), 1, 0)
            scale = lax.rsqrt(jnp.mean(result * result, axis=1, keepdims=True) + EPS)
            hidden[:, cols(j)] = (result * scale * gated[j]).astype(BF16)
        return carry

    lax.fori_loop(0, HALF // 4, finish, 0)

    def p_copy(block):
        return remote(
            p_send.at[block], p_recv.at[block], ps_sem.at[block], pr_sem.at[block], partner, dp
        )

    def project(block):
        rhs = jnp.concatenate([w_buf[2 * block], w_buf[2 * block + 1]], axis=1)
        p_buf[block] = dot(hidden[...], rhs, 1, 0)
        p_send[block] = p_buf[block, their_rows, :].astype(BF16)
        p_copy(block).start()

    w_swap.wait_recv()
    project(y)

    def project_far(slot, carry):
        way, s = lax.div(slot, 3), lax.rem(slot, 3) + 1
        step = jnp.where(slot == 6, 4, jnp.where(way == 0, NY - s, s))
        block = lax.rem(y + step, NY)
        for piece in range(2):
            for copy in spread_copies(piece, slot, block):
                copy.wait_recv()
        project(block)
        return carry

    lax.fori_loop(0, NY - 1, project_far, 0)

    def gather(i, carry):
        for t in range(2):
            block = 2 * i + t
            p_copy(block).wait_recv()
            at = pl.ds(pl.multiple_of(block * SPAN, SPAN), SPAN)
            total = p_buf[block, my_rows, :] + p_recv[block].astype(F32)
            out_ref[0, :, at] = total.astype(BF16)
        return carry

    lax.fori_loop(0, NY // 2, gather, 0)

    for copy in swaps:
        copy.wait_send()
    w_swap.wait_send()

    def drain_decay(to_y, carry):
        to, copy = decay_copy(to_y)

        @pl.when(to != sp)
        def _():
            copy.wait_send()

        return carry

    def drain_g(j, carry):
        @pl.when(jnp.logical_and(HALF * c + j != sp, y != NY - 1))
        def _():
            g_copy(j).wait_send()

        return carry

    def drain_s(to_y, carry):
        to, copy = s_copy(to_y)

        @pl.when(to != sp)
        def _():
            copy.wait_send()

        return carry

    def drain_spread(slot, carry):
        for piece in range(2):
            for copy in spread_copies(piece, slot, y):
                copy.wait_send()
        return carry

    def drain_p(block, carry):
        p_copy(block).wait_send()
        return carry

    lax.fori_loop(0, NY, drain_decay, 0)
    lax.fori_loop(0, HALF, drain_g, 0)
    lax.fori_loop(1, NY, drain_s, 0)
    for piece in range(2):
        for way in range(2):
            for lane in range(2):
                first_copy(way, piece, lane).wait_send()
                for s in (2, 3, 4):
                    if s < 4 or piece == way:
                        hop_copy(way, piece, lane, s).wait_send()
    lax.fori_loop(0, NY - 1, drain_spread, 0)
    lax.fori_loop(0, NY, drain_p, 0)


def on_device(q, k, v, gates, log_decay, weight):
    dma = pltpu.SemaphoreType.DMA
    vmem = pltpu.VMEM
    state_shape = (NY, SIZE, SIZE)
    return pl.pallas_call(
        kernel,
        out_shape=pltpu.VMEM(q.shape, BF16),
        in_specs=[pl.BlockSpec(memory_space=pltpu.HBM)] * 6,
        out_specs=pl.BlockSpec(memory_space=pltpu.VMEM),
        scratch_shapes=[
            vmem((4, SPAN, LANE), BF16),
            vmem((1, NY * SPAN), F32),
            vmem((HALF, 1, SPAN), F32),
            vmem((2 * LANE, SIZE), BF16),
            vmem((HEADS, LANE, SIZE), BF16),
            vmem((SPAN, SIZE), F32),
            vmem((SPAN, SIZE), F32),
            vmem((SPAN, SPAN), BF16),
            vmem((HALF, SPAN, SIZE), F32),
            vmem((HALF, 1, SPAN), F32),
            vmem((HALF, 1, SPAN), F32),
            vmem((NY, 1, SIZE), F32),
            vmem((HALF, SIZE, SPAN), F32),
            vmem((HALF, SPAN, SIZE), F32),
            vmem((HALF, SPAN, SPAN), BF16),
            vmem((HALF, SPAN, SIZE), F32),
            vmem(state_shape, BF16),
            vmem(state_shape, BF16),
            vmem(state_shape, BF16),
            vmem(state_shape, BF16),
            vmem((SIZE, SIZE), F32),
            vmem((SPAN, LANE), BF16),
            vmem((NY, SPAN, SPAN), F32),
            vmem((NY, TOK, SPAN), BF16),
            vmem((NY, TOK, SPAN), BF16),
            dma((4,)),
            dma,
            dma,
            dma((4,)),
            dma((4,)),
            dma((NY,)),
            dma((HALF,)),
            dma,
            dma,
            dma((2, 2, 2)),
            dma((2, 2, 2, 5)),
            dma((2, 2, 2, 5)),
            dma((2, 4, NY - 1)),
            dma((2, 4, NY - 1)),
            dma((HALF,)),
            dma((NY,)),
            dma((NY,)),
            dma((HALF,)),
            dma((NY,)),
            dma((NY,)),
        ],
        compiler_params=pltpu.CompilerParams(
            collective_id=0, has_side_effects=True, vmem_limit_bytes=60 * 1024 * 1024
        ),
        name="retention",
    )(q, k, v, gates, log_decay, weight)


def solution(mesh):
    placed = (P("dp", "sp", None),) * 5 + (P(None, "sp"),)
    return jax.shard_map(
        on_device, mesh=mesh, in_specs=placed, out_specs=P("dp", "sp", None), check_vma=False
    )
```
